32 devices in a mesh: fs: 16 (over z, x, core), tp: 2 (over y).
Axes of the slice: x: 2, y: 2, z: 4, core: 2. Of those that a mesh axis runs over, the one named last changes fastest.
Arguments:
- normed_input: bfloat16 [8192, 2048], P('fs'), may hold values from -6 to 6
- value_cotangent: bfloat16 [8192, 2048], P('fs', 'tp'), may hold values from -6 to 6
- gated_output: bfloat16 [8192, 2048], P('fs', 'tp'), may hold values from -6 to 6
- layer_cotangent: bfloat16 [8192, 2048], P('fs'), may hold values from -6 to 6
- factor_value: bfloat16 [2048, 256], P('fs'), may hold values from -4 to 4, as said below
- factor_output: bfloat16 [2048, 256], P('fs'), may hold values from -4 to 4, as said below
- weight_value: float32 [2048, 2048], P('fs', 'tp'), may hold values from -0.125 to 0.125
- weight_output: float32 [2048, 2048], P('tp', 'fs'), may hold values from -0.125 to 0.125
- first_value: float32 [256, 2048], P('fs', 'tp'), may hold values from -2048 to 2048
- second_value: float32 [256, 2048], P('fs', 'tp'), may hold values from 32768 to 524288
- first_output: float32 [256, 2048], P('fs', 'tp'), may hold values from -2048 to 2048
- second_output: float32 [256, 2048], P('fs', 'tp'), may hold values from 32768 to 524288
Outputs:
- step_value: float32 [2048, 2048], P('fs', 'tp')
- step_output: float32 [2048, 2048], P('tp', 'fs')
- next_weight_value: float32 [2048, 2048], P('fs', 'tp')
- next_weight_output: float32 [2048, 2048], P('tp', 'fs')
- next_first_value: float32 [256, 2048], P('fs', 'tp')
- next_second_value: float32 [256, 2048], P('fs', 'tp')
- next_first_output: float32 [256, 2048], P('fs', 'tp')
- next_second_output: float32 [256, 2048], P('fs', 'tp')
- copy_value: bfloat16 [2048, 2048], P(None, 'tp')
- copy_output: bfloat16 [2048, 2048], P('tp')
The draws below stay inside these ranges and needn't reach their ends.
Inputs may be any that keep to these rules, and one draw needn't show every extreme that they name: factor_value has full rank. factor_output has full rank.
All inputs are finite; a program needn't handle non-finite values.
Results may differ from the reference program's by a relative error of at most 0.0039.
Values may be sent and summed in bfloat16 or wider, within the bound.
A program may use at most 64 MiB of HBM per device.

```python
import math
import jax
import jax.numpy as jnp
from jax import lax

D = 2048
WIDTH = 2048
R = 256
TOKENS = 8192


def make_factor(key):
    rising = jnp.exp(jnp.log(10.0) * jnp.arange(D, dtype=jnp.float32) / D)
    base = jnp.clip(jax.random.normal(key, (D, R), jnp.float32), -6.0, 6.0)
    return (base * rising[:, None] / jnp.sqrt(jnp.float32(D))).astype(jnp.bfloat16)


def draw_factor_value(key, part):
    return make_factor(jax.random.fold_in(key, 11))


def draw_factor_output(key, part):
    return make_factor(jax.random.fold_in(key, 17))


def shard_levels(key, dims, split, low, high):
    gain, own = 1.0, jax.random.fold_in(key, 6)
    for position, parts in split:
        heights = jnp.exp(jax.random.uniform(jax.random.fold_in(own, position), (parts,), jnp.float32, low / len(split), high / len(split)))
        gain = gain * jnp.repeat(heights, dims[position] // parts).reshape([-1 if axis == position else 1 for axis in range(len(dims))])
    return gain


def scatter_about(own_key, shape, scale, limit, pieces=(), held_as=jnp.bfloat16):
    array = scale * jax.random.normal(own_key, shape, jnp.float32)
    if pieces:
        array = array * shard_levels(own_key, shape, pieces, -0.22, 0.18)
    return jnp.clip(array, -limit, limit).astype(held_as)


def setup_inputs(seed: int = 0) -> dict:
    keys = jax.random.split(jax.random.key(seed), 13)
    normed_input = scatter_about(keys[0], (TOKENS, D), 1.0, 6.0, ((0, 16),))
    value_cotangent = scatter_about(keys[1], (TOKENS, WIDTH), 1.0, 6.0, ((0, 16), (1, 2)))
    gated_output = scatter_about(keys[2], (TOKENS, WIDTH), 1.0, 6.0, ((0, 16), (1, 2)))
    layer_cotangent = scatter_about(keys[3], (TOKENS, D), 1.0, 6.0, ((0, 16),))
    factor_value = draw_factor_value(jax.random.fold_in(keys[12], 71), 0)
    factor_output = draw_factor_output(jax.random.fold_in(keys[12], 71), 0)
    weight_value = scatter_about(keys[6], (D, WIDTH), D ** -0.5, 0.125, ((0, 16), (1, 2)), jnp.float32)
    weight_output = scatter_about(keys[7], (WIDTH, D), WIDTH ** -0.5, 0.125, ((0, 2), (1, 16)), jnp.float32)
    first_value = scatter_about(keys[8], (R, WIDTH), (4 * TOKENS ** 0.5), 2048.0, ((0, 16), (1, 2)), jnp.float32)
    second_value = jnp.clip(jnp.exp(math.log(524288.0) - 2.7725887 * jax.random.uniform(keys[9], (R, WIDTH), jnp.float32) ** shard_levels(keys[9], (R, WIDTH), ((0, 16), (1, 2)), -0.2, 0.2)), 32768.0, 524288.0)
    first_output = scatter_about(keys[10], (R, WIDTH), (4 * TOKENS ** 0.5), 2048.0, ((0, 16), (1, 2)), jnp.float32)
    second_output = jnp.clip(jnp.exp(math.log(524288.0) - 2.7725887 * jax.random.uniform(keys[11], (R, WIDTH), jnp.float32) ** shard_levels(keys[11], (R, WIDTH), ((0, 16), (1, 2)), -0.2, 0.2)), 32768.0, 524288.0)
    return dict(normed_input=normed_input, value_cotangent=value_cotangent, gated_output=gated_output, layer_cotangent=layer_cotangent, factor_value=factor_value, factor_output=factor_output, weight_value=weight_value, weight_output=weight_output, first_value=first_value, second_value=second_value, first_output=first_output, second_output=second_output)


def reference(normed_input, value_cotangent, gated_output, layer_cotangent, factor_value, factor_output, weight_value, weight_output, first_value, second_value, first_output, second_output):
    projected_input = jnp.dot(normed_input, factor_value, preferred_element_type=jnp.float32).astype(jnp.bfloat16)
    projected_cotangent = jnp.dot(layer_cotangent, factor_output, preferred_element_type=jnp.float32).astype(jnp.bfloat16)
    low_value = jnp.dot(projected_input.T, value_cotangent, preferred_element_type=jnp.float32)
    low_output = jnp.dot(projected_cotangent.T, gated_output, preferred_element_type=jnp.float32)
    next_first_value = 0.9 * first_value + 0.1 * low_value
    next_second_value = 0.95 * second_value + 0.05 * low_value * low_value
    next_first_output = 0.9 * first_output + 0.1 * low_output
    next_second_output = 0.95 * second_output + 0.05 * low_output * low_output
    direction_value = (next_first_value * lax.rsqrt(next_second_value)).astype(jnp.bfloat16)
    direction_output = (next_first_output * lax.rsqrt(next_second_output)).astype(jnp.bfloat16)
    update_value = jnp.dot(factor_value, direction_value, preferred_element_type=jnp.float32)
    update_output = jnp.dot(direction_output.T, factor_output.T, preferred_element_type=jnp.float32)
    entries = D * WIDTH
    total_value = jnp.sum(update_value * update_value)
    total_output = jnp.sum(update_output * update_output)
    step_value = update_value * lax.rsqrt(total_value / entries + 1e-06)
    step_output = update_output * lax.rsqrt(total_output / entries + 1e-06)
    next_weight_value = weight_value - 0.02 * step_value
    next_weight_output = weight_output - 0.02 * step_output
    return (step_value, step_output, next_weight_value, next_weight_output, next_first_value, next_second_value, next_first_output, next_second_output, next_weight_value.astype(jnp.bfloat16), next_weight_output.astype(jnp.bfloat16))
```

```python
import functools

import jax
import jax.numpy as jnp
from jax import lax
from jax.experimental import pallas as pl
from jax.experimental.pallas import tpu as pltpu
from jax.sharding import PartitionSpec as P

CORES = 2

D = 2048
WIDTH = 2048


def gram_times(gram_matrix, directions):
    gram_high = gram_matrix.astype(jnp.bfloat16)
    gram_low = (gram_matrix - gram_high.astype(jnp.float32)).astype(jnp.bfloat16)
    return jnp.dot(gram_high, directions, preferred_element_type=jnp.float32) + jnp.dot(
        gram_low, directions, preferred_element_type=jnp.float32
    )


def body(
    normed_input,
    value_cotangent,
    gated_output,
    layer_cotangent,
    factor_value,
    factor_output,
    weight_value,
    weight_output,
    first_value,
    second_value,
    first_output,
    second_output,
):
    col_count = value_cotangent.shape[1]
    inner = (((0,), (0,)), ((), ()))
    pieces = (
        lax.all_gather(factor_value, "fs", axis=0, tiled=True),
        lax.all_gather(factor_output, "fs", axis=0, tiled=True),
    )
    piece_value, piece_output = pieces
    span_input = normed_input
    span_cotan = layer_cotangent
    gram_value = lax.dot_general(pieces[0], pieces[0], inner, preferred_element_type=jnp.float32)
    gram_output = lax.dot_general(pieces[1], pieces[1], inner, preferred_element_type=jnp.float32)
    projected_input = jnp.dot(span_input, piece_value, preferred_element_type=jnp.float32).astype(
        jnp.bfloat16
    )
    projected_cotangent = jnp.dot(
        span_cotan, piece_output, preferred_element_type=jnp.float32
    ).astype(jnp.bfloat16)
    span_input = projected_input
    span_cotan = projected_cotangent
    term_value = lax.dot_general(
        span_input, value_cotangent, inner, preferred_element_type=jnp.float32
    )
    term_output = lax.dot_general(
        span_cotan, gated_output, inner, preferred_element_type=jnp.float32
    )
    low_rank = lax.psum_scatter(
        jnp.concatenate([term_value, term_output], axis=1), "fs", scatter_dimension=0, tiled=True
    )
    low_value = low_rank[:, :col_count]
    low_output = low_rank[:, col_count:]
    next_first_value = 0.9 * first_value + 0.1 * low_value
    next_second_value = 0.95 * second_value + 0.05 * low_value * low_value
    next_first_output = 0.9 * first_output + 0.1 * low_output
    next_second_output = 0.95 * second_output + 0.05 * low_output * low_output
    direction_value = (next_first_value * lax.rsqrt(next_second_value)).astype(jnp.bfloat16)
    direction_output = (next_first_output * lax.rsqrt(next_second_output)).astype(jnp.bfloat16)
    gathered_value, gathered_output = (
        lax.all_gather(direction_value, "fs", axis=0, tiled=True),
        lax.all_gather(direction_output, "fs", axis=0, tiled=True),
    )
    update_value = jnp.dot(factor_value, gathered_value, preferred_element_type=jnp.float32)
    update_output = lax.dot_general(
        gathered_output, factor_output, (((0,), (1,)), ((), ())), preferred_element_type=jnp.float32
    )
    square_value = jnp.sum(
        gathered_value.astype(jnp.float32) * gram_times(gram_value, gathered_value)
    )
    square_output = jnp.sum(
        gathered_output.astype(jnp.float32) * gram_times(gram_output, gathered_output)
    )
    total_value, total_output = lax.psum((square_value, square_output), "tp")
    entries = D * WIDTH
    step_value = update_value * lax.rsqrt(total_value / entries + 1e-06)
    step_output = update_output * lax.rsqrt(total_output / entries + 1e-06)
    next_weight_value = weight_value - 0.02 * step_value
    next_weight_output = weight_output - 0.02 * step_output
    half_value = next_weight_value.astype(jnp.bfloat16)
    half_output = next_weight_output.astype(jnp.bfloat16)
    copy_value, copy_output = (
        lax.all_gather(half_value, "fs", axis=0, tiled=True),
        lax.all_gather(half_output, "fs", axis=1, tiled=True),
    )
    return (
        step_value,
        step_output,
        next_weight_value,
        next_weight_output,
        next_first_value,
        next_second_value,
        next_first_output,
        next_second_output,
        copy_value,
        copy_output,
    )


class Relay:
    def __init__(self, place, block, send_sem, recv_sem):
        self.z, self.x, self.core, self.depth, self.width = place
        self.block, self.send_sem, self.recv_sem = block, send_sem, recv_sem
        self.pending = []

    def index(self, shift, x, core):
        z = lax.rem(self.z + shift, self.depth)
        return (z * self.width + x) * CORES + core

    def copy(self, origin, target, slot):
        return pltpu.make_async_remote_copy(
            src_ref=self.block(origin),
            dst_ref=self.block(origin),
            send_sem=self.send_sem.at[slot],
            recv_sem=self.recv_sem.at[origin],
            device_id={"fs": target},
            device_id_type=pl.DeviceIdType.MESH,
        )

    def send(self, origin, target):
        copy = self.copy(origin, target, len(self.pending))
        copy.start()
        self.pending.append(copy)

    def arrived(self, origin):
        self.copy(origin, self.index(0, self.x, 1 - self.core), 0).wait_recv()

    def over_x(self, origin):
        self.send(origin, self.index(0, 1 - self.x, self.core))

    def over_core(self, origin):
        self.send(origin, self.index(0, self.x, 1 - self.core))

    def order(self):
        shifts = []
        for hop in range(1, self.depth // 2 + 1):
            for shift in (hop, self.depth - hop):
                if shift not in shifts:
                    shifts.append(shift)
        return shifts

    def begin(self):
        own = self.index(0, self.x, self.core)
        for shift in self.order():
            self.send(own, self.index(shift, self.x, self.core))
        self.over_x(own)
        self.over_core(own)

    def along_z(self, shift):
        origin = self.index(shift, self.x, self.core)
        self.arrived(origin)
        self.over_x(origin)
        self.over_core(origin)

    def across(self, shift):
        origin = self.index(shift, 1 - self.x, self.core)
        self.arrived(origin)
        self.over_core(origin)

    def middle(self):
        lagged = [0]
        for shift in self.order():
            yield functools.partial(self.along_z, shift)
            lagged.append(shift)
            if len(lagged) > 1:
                yield functools.partial(self.across, lagged.pop(0))
        for shift in lagged:
            yield functools.partial(self.across, shift)

    def finish(self):
        for shift in [0] + self.order():
            for x in (self.x, 1 - self.x):
                self.arrived(self.index(shift, x, 1 - self.core))
        for copy in self.pending:
            copy.wait_send()


def fused(
    fs_size,
    tp_size,
    input_hbm,
    value_hbm,
    gated_hbm,
    layer_hbm,
    factor_value_hbm,
    factor_output_hbm,
    weight_value_ref,
    weight_output_ref,
    first_value_ref,
    second_value_ref,
    first_output_ref,
    second_output_ref,
    step_value_ref,
    step_output_ref,
    next_weight_value_ref,
    next_weight_output_ref,
    next_first_value_ref,
    next_second_value_ref,
    next_first_output_ref,
    next_second_output_ref,
    copy_value_ref,
    copy_output_ref,
    stream,
    cotan,
    factors,
    projected,
    terms,
    paired,
    outgoing,
    incoming,
    directions,
    totals,
    load_sem,
    pair_send,
    pair_recv,
    sum_send,
    sum_recv,
    total_send,
    total_recv,
    relay_send,
    relay_recv,
):
    fs, tp = lax.axis_index("fs"), lax.axis_index("tp")
    width = tp_size
    chips = fs_size // CORES
    depth = chips // width
    core, chip = lax.rem(fs, CORES), fs // CORES
    x, z = lax.rem(chip, width), chip // width
    place = (z, x, core, depth, width)
    partner = chip * CORES + 1 - core
    mesh_id = pl.DeviceIdType.MESH
    rows = factor_value_hbm.shape[0]
    tokens = input_hbm.shape[0]
    cols = value_hbm.shape[1]
    ranks = first_value_ref.shape[0]
    everyone = [(a, b) for a in range(fs_size) for b in range(tp_size)][1:]

    own_rows = pl.ds(pl.multiple_of(fs * rows, rows), rows)
    loads = [
        pltpu.make_async_copy(source, target, load_sem.at[slot])
        for slot, (source, target) in enumerate(
            (
                (factor_value_hbm, factors.at[0, own_rows]),
                (factor_output_hbm, factors.at[1, own_rows]),
                (input_hbm, stream.at[0]),
                (layer_hbm, stream.at[1]),
                (value_hbm, cotan.at[0]),
                (gated_hbm, cotan.at[1]),
            )
        )
    ]
    for load in loads:
        load.start()

    barrier = pltpu.get_barrier_semaphore()
    for a, b in everyone:
        pl.semaphore_signal(
            barrier,
            inc=1,
            device_id={"fs": lax.rem(fs + a, fs_size), "tp": lax.rem(tp + b, tp_size)},
            device_id_type=mesh_id,
        )
    loads[0].wait()
    loads[1].wait()
    pl.semaphore_wait(barrier, len(everyone))

    def row_block(ref, size, lead=False):
        def block(origin):
            span = pl.ds(pl.multiple_of(origin * size, size), size)
            return ref.at[:, span] if lead else ref.at[span]

        return block

    def column_block(origin):
        return copy_output_ref.at[:, pl.ds(pl.multiple_of(origin * rows, rows), rows)]

    relays = [
        Relay(place, block, relay_send.at[slot], relay_recv.at[slot])
        for slot, block in enumerate(
            (
                row_block(factors, rows, True),
                row_block(directions, ranks),
                row_block(copy_value_ref, rows),
                column_block,
            )
        )
    ]

    relays[0].begin()
    for step in relays[0].middle():
        step()
    relays[0].finish()
    for load in loads[2:]:
        load.wait()

    tile = 128
    for kind in range(2):

        @pl.loop(0, tokens // tile)
        def _(step, kind=kind):
            span = pl.ds(pl.multiple_of(step * tile, tile), tile)
            projected[kind, span] = jnp.dot(
                stream[kind, span], factors[kind], preferred_element_type=jnp.float32
            ).astype(jnp.bfloat16)

    width_tile = 256
    for kind in range(2):

        @pl.loop(0, cols // width_tile)
        def _(step, kind=kind):
            span = pl.ds(pl.multiple_of(step * width_tile, width_tile), width_tile)
            term = lax.dot_general(
                projected[kind],
                cotan[kind, :, span],
                (((0,), (0,)), ((), ())),
                preferred_element_type=jnp.float32,
            )
            target = pl.ds(pl.multiple_of(kind * cols + step * width_tile, width_tile), width_tile)
            terms[:, :, :, target] = term.reshape(chips, CORES, ranks, width_tile)

    pairs = []
    for shift in list(range(1, chips)) + [0]:
        c = lax.rem(chip + shift, chips)
        copy = pltpu.make_async_remote_copy(
            src_ref=terms.at[c, 1 - core],
            dst_ref=paired.at[c],
            send_sem=pair_send.at[shift],
            recv_sem=pair_recv.at[c],
            device_id={"fs": partner},
            device_id_type=mesh_id,
        )
        copy.start()
        pairs.append(copy)
    sums = []
    for shift in range(1, chips):
        c = lax.rem(chip + shift, chips)
        pairs[shift - 1].wait_recv()
        outgoing[c] = (terms[c, core] + paired[c]).astype(jnp.bfloat16)
        copy = pltpu.make_async_remote_copy(
            src_ref=outgoing.at[c],
            dst_ref=incoming.at[chip],
            send_sem=sum_send.at[shift],
            recv_sem=sum_recv.at[chip],
            device_id={"fs": c * CORES + core},
            device_id_type=mesh_id,
        )
        copy.start()
        sums.append(copy)
    pairs[-1].wait_recv()
    low = terms[chip, core] + paired[chip]
    for shift in range(1, chips):
        c = lax.rem(chip + chips - shift, chips)
        pltpu.make_async_remote_copy(
            src_ref=outgoing.at[c],
            dst_ref=incoming.at[c],
            send_sem=sum_send.at[shift],
            recv_sem=sum_recv.at[c],
            device_id={"fs": c * CORES + core},
            device_id_type=mesh_id,
        ).wait_recv()
        low = low + incoming[c].astype(jnp.float32)

    own_ranks = pl.ds(pl.multiple_of(fs * ranks, ranks), ranks)
    moments = (
        (first_value_ref, second_value_ref, next_first_value_ref, next_second_value_ref),
        (first_output_ref, second_output_ref, next_first_output_ref, next_second_output_ref),
    )
    for kind, (first_ref, second_ref, next_first_ref, next_second_ref) in enumerate(moments):
        part = low[:, kind * cols : (kind + 1) * cols]
        next_first = 0.9 * first_ref[...] + 0.1 * part
        next_second = 0.95 * second_ref[...] + 0.05 * part * part
        next_first_ref[...] = next_first
        next_second_ref[...] = next_second
        directions[own_ranks, kind * cols : (kind + 1) * cols] = (
            next_first * lax.rsqrt(next_second)
        ).astype(jnp.bfloat16)
    relays[1].begin()
    for step in relays[1].middle():
        step()
    relays[1].finish()

    me = fs * tp_size + tp
    for kind, step_ref in enumerate((step_value_ref, step_output_ref)):
        square = jnp.zeros((8, 128), jnp.float32)
        for start in range(0, cols, width_tile):
            update = jnp.dot(
                factors[kind, own_rows],
                directions[:, kind * cols + start : kind * cols + start + width_tile],
                preferred_element_type=jnp.float32,
            )
            if kind == 0:
                step_ref[:, start : start + width_tile] = update
            else:
                step_ref[start : start + width_tile, :] = update.T
            fold = jnp.sum((update * update).reshape(rows // 8, 8, width_tile), axis=0)
            for lane in range(0, width_tile, 128):
                square = square + fold[:, lane : lane + 128]
        totals[me, kind] = square
    shares = []
    for slot, (a, b) in enumerate(everyone):
        copy = pltpu.make_async_remote_copy(
            src_ref=totals.at[me],
            dst_ref=totals.at[me],
            send_sem=total_send.at[slot],
            recv_sem=total_recv.at[me],
            device_id={"fs": lax.rem(fs + a, fs_size), "tp": lax.rem(tp + b, tp_size)},
            device_id_type=mesh_id,
        )
        copy.start()
        shares.append(copy)
    for a, b in everyone:
        other_fs, other_tp = lax.rem(fs + a, fs_size), lax.rem(tp + b, tp_size)
        other = other_fs * tp_size + other_tp
        pltpu.make_async_remote_copy(
            src_ref=totals.at[other],
            dst_ref=totals.at[other],
            send_sem=total_send.at[0],
            recv_sem=total_recv.at[other],
            device_id={"fs": other_fs, "tp": other_tp},
            device_id_type=mesh_id,
        ).wait_recv()
    entries = rows * fs_size * cols * tp_size
    scales = []
    for kind in range(2):
        total = jnp.sum(jnp.sum(totals[:, kind], axis=0), keepdims=True)
        scales.append(lax.rsqrt(total / entries + 1e-06))

    step_value = step_value_ref[...] * scales[0]
    next_weight = weight_value_ref[...] - 0.02 * step_value
    step_value_ref[...] = step_value
    next_weight_value_ref[...] = next_weight
    copy_value_ref[own_rows, :] = next_weight.astype(jnp.bfloat16)
    relays[2].begin()
    step_output = step_output_ref[...] * scales[1]
    next_weight = weight_output_ref[...] - 0.02 * step_output
    step_output_ref[...] = step_output
    next_weight_output_ref[...] = next_weight
    copy_output_ref[:, own_rows] = next_weight.astype(jnp.bfloat16)
    relays[3].begin()
    for first, second in zip(relays[2].middle(), relays[3].middle()):
        first()
        second()
    relays[2].finish()
    relays[3].finish()
    for copy in pairs + sums + shares:
        copy.wait_send()


def fused_body(fs_size, tp_size, *args):
    tokens, model = args[0].shape
    cols = args[1].shape[1]
    rows, rank = args[4].shape
    ranks = args[8].shape[0]
    chips = fs_size // CORES
    f32, bf16 = jnp.float32, jnp.bfloat16
    vmem, anywhere = pl.BlockSpec(memory_space=pltpu.VMEM), pl.BlockSpec(memory_space=pl.ANY)
    shape = jax.ShapeDtypeStruct
    hops = chips // tp_size - 1 + chips // tp_size + chips
    dma = pltpu.SemaphoreType.DMA
    return pl.pallas_call(
        functools.partial(fused, fs_size, tp_size),
        out_shape=(
            [shape((rows, cols), f32), shape((cols, rows), f32)] * 2
            + [shape((ranks, cols), f32)] * 4
            + [shape((model, cols), bf16), shape((cols, model), bf16)]
        ),
        in_specs=[anywhere] * 6 + [vmem] * 6,
        out_specs=[vmem] * 10,
        scratch_shapes=[
            pltpu.VMEM((2, tokens, model), bf16),
            pltpu.VMEM((2, tokens, cols), bf16),
            pltpu.VMEM((2, model, rank), bf16),
            pltpu.VMEM((2, tokens, rank), bf16),
            pltpu.VMEM((chips, CORES, ranks, 2 * cols), f32),
            pltpu.VMEM((chips, ranks, 2 * cols), f32),
            pltpu.VMEM((chips, ranks, 2 * cols), bf16),
            pltpu.VMEM((chips, ranks, 2 * cols), bf16),
            pltpu.VMEM((rank, 2 * cols), bf16),
            pltpu.VMEM((fs_size * tp_size, 2, 8, 128), f32),
            dma((6,)),
            dma((chips,)),
            dma((chips,)),
            dma((chips,)),
            dma((chips,)),
            dma((fs_size * tp_size,)),
            dma((fs_size * tp_size,)),
            dma((4, hops)),
            dma((4, fs_size)),
        ],
        compiler_params=pltpu.CompilerParams(
            collective_id=0, has_side_effects=True, vmem_limit_bytes=60 * 1024 * 1024
        ),
    )(*args)


def solution(mesh):
    fs_size, tp_size = mesh.shape["fs"], mesh.shape["tp"]
    placed = (
        P("fs", None),
        P("fs", "tp"),
        P("fs", "tp"),
        P("fs", None),
        P("fs", None),
        P("fs", None),
        P("fs", "tp"),
        P("tp", "fs"),
        P("fs", "tp"),
        P("fs", "tp"),
        P("fs", "tp"),
        P("fs", "tp"),
    )
    chips = fs_size // CORES
    tiled = tp_size == 2 and fs_size == 16 and chips % tp_size == 0
    return jax.shard_map(
        functools.partial(fused_body, fs_size, tp_size) if tiled else body,
        mesh=mesh,
        in_specs=placed,
        out_specs=(
            P("fs", "tp"),
            P("tp", "fs"),
            P("fs", "tp"),
            P("tp", "fs"),
            P("fs", "tp"),
            P("fs", "tp"),
            P("fs", "tp"),
            P("fs", "tp"),
            P(None, "tp"),
            P("tp", None),
        ),
        check_vma=False,
    )
```

```python
import functools

import jax
import jax.numpy as jnp
from jax import lax
from jax.experimental import pallas as pl
from jax.experimental.pallas import tpu as pltpu
from jax.sharding import PartitionSpec as P

CORES = 2

D = 2048
WIDTH = 2048


def gram_times(gram_matrix, directions):
    gram_high = gram_matrix.astype(jnp.bfloat16)
    gram_low = (gram_matrix - gram_high.astype(jnp.float32)).astype(jnp.bfloat16)
    return jnp.dot(gram_high, directions, preferred_element_type=jnp.float32) + jnp.dot(
        gram_low, directions, preferred_element_type=jnp.float32
    )


def body(
    normed_input,
    value_cotangent,
    gated_output,
    layer_cotangent,
    factor_value,
    factor_output,
    weight_value,
    weight_output,
    first_value,
    second_value,
    first_output,
    second_output,
):
    col_count = value_cotangent.shape[1]
    inner = (((0,), (0,)), ((), ()))
    pieces = (
        lax.all_gather(factor_value, "fs", axis=0, tiled=True),
        lax.all_gather(factor_output, "fs", axis=0, tiled=True),
    )
    piece_value, piece_output = pieces
    span_input = normed_input
    span_cotan = layer_cotangent
    gram_value = lax.dot_general(pieces[0], pieces[0], inner, preferred_element_type=jnp.float32)
    gram_output = lax.dot_general(pieces[1], pieces[1], inner, preferred_element_type=jnp.float32)
    projected_input = jnp.dot(span_input, piece_value, preferred_element_type=jnp.float32).astype(
        jnp.bfloat16
    )
    projected_cotangent = jnp.dot(
        span_cotan, piece_output, preferred_element_type=jnp.float32
    ).astype(jnp.bfloat16)
    span_input = projected_input
    span_cotan = projected_cotangent
    term_value = lax.dot_general(
        span_input, value_cotangent, inner, preferred_element_type=jnp.float32
    )
    term_output = lax.dot_general(
        span_cotan, gated_output, inner, preferred_element_type=jnp.float32
    )
    low_rank = lax.psum_scatter(
        jnp.concatenate([term_value, term_output], axis=1), "fs", scatter_dimension=0, tiled=True
    )
    low_value = low_rank[:, :col_count]
    low_output = low_rank[:, col_count:]
    next_first_value = 0.9 * first_value + 0.1 * low_value
    next_second_value = 0.95 * second_value + 0.05 * low_value * low_value
    next_first_output = 0.9 * first_output + 0.1 * low_output
    next_second_output = 0.95 * second_output + 0.05 * low_output * low_output
    direction_value = (next_first_value * lax.rsqrt(next_second_value)).astype(jnp.bfloat16)
    direction_output = (next_first_output * lax.rsqrt(next_second_output)).astype(jnp.bfloat16)
    gathered_value, gathered_output = (
        lax.all_gather(direction_value, "fs", axis=0, tiled=True),
        lax.all_gather(direction_output, "fs", axis=0, tiled=True),
    )
    update_value = jnp.dot(factor_value, gathered_value, preferred_element_type=jnp.float32)
    update_output = lax.dot_general(
        gathered_output, factor_output, (((0,), (1,)), ((), ())), preferred_element_type=jnp.float32
    )
    square_value = jnp.sum(
        gathered_value.astype(jnp.float32) * gram_times(gram_value, gathered_value)
    )
    square_output = jnp.sum(
        gathered_output.astype(jnp.float32) * gram_times(gram_output, gathered_output)
    )
    total_value, total_output = lax.psum((square_value, square_output), "tp")
    entries = D * WIDTH
    step_value = update_value * lax.rsqrt(total_value / entries + 1e-06)
    step_output = update_output * lax.rsqrt(total_output / entries + 1e-06)
    next_weight_value = weight_value - 0.02 * step_value
    next_weight_output = weight_output - 0.02 * step_output
    half_value = next_weight_value.astype(jnp.bfloat16)
    half_output = next_weight_output.astype(jnp.bfloat16)
    copy_value, copy_output = (
        lax.all_gather(half_value, "fs", axis=0, tiled=True),
        lax.all_gather(half_output, "fs", axis=1, tiled=True),
    )
    return (
        step_value,
        step_output,
        next_weight_value,
        next_weight_output,
        next_first_value,
        next_second_value,
        next_first_output,
        next_second_output,
        copy_value,
        copy_output,
    )


class Relay:
    def __init__(self, place, block, send_sem, recv_sem):
        self.z, self.x, self.core, self.depth, self.width = place
        self.block, self.send_sem, self.recv_sem = block, send_sem, recv_sem
        self.pending = []

    def index(self, shift, x, core):
        z = lax.rem(self.z + shift, self.depth)
        return (z * self.width + x) * CORES + core

    def copy(self, origin, target, slot):
        return pltpu.make_async_remote_copy(
            src_ref=self.block(origin),
            dst_ref=self.block(origin),
            send_sem=self.send_sem.at[slot],
            recv_sem=self.recv_sem.at[origin],
            device_id={"fs": target},
            device_id_type=pl.DeviceIdType.MESH,
        )

    def send(self, origin, target):
        copy = self.copy(origin, target, len(self.pending))
        copy.start()
        self.pending.append(copy)

    def arrived(self, origin):
        self.copy(origin, self.index(0, self.x, 1 - self.core), 0).wait_recv()

    def over_x(self, origin):
        self.send(origin, self.index(0, 1 - self.x, self.core))

    def over_core(self, origin):
        self.send(origin, self.index(0, self.x, 1 - self.core))

    def order(self):
        shifts = []
        for hop in range(1, self.depth // 2 + 1):
            for shift in (hop, self.depth - hop):
                if shift not in shifts:
                    shifts.append(shift)
        return shifts

    def begin(self):
        own = self.index(0, self.x, self.core)
        for shift in self.order():
            self.send(own, self.index(shift, self.x, self.core))
        self.over_x(own)
        self.over_core(own)

    def along_z(self, shift):
        origin = self.index(shift, self.x, self.core)
        self.arrived(origin)
        self.over_x(origin)
        self.over_core(origin)

    def across(self, shift):
        origin = self.index(shift, 1 - self.x, self.core)
        self.arrived(origin)
        self.over_core(origin)

    def middle(self):
        lagged = [0]
        for shift in self.order():
            yield functools.partial(self.along_z, shift)
            lagged.append(shift)
            if len(lagged) > 1:
                yield functools.partial(self.across, lagged.pop(0))
        for shift in lagged:
            yield functools.partial(self.across, shift)

    def finish(self):
        for shift in [0] + self.order():
            for x in (self.x, 1 - self.x):
                self.arrived(self.index(shift, x, 1 - self.core))
        for copy in self.pending:
            copy.wait_send()


def next_moments(first, second, low):
    return 0.9 * first + 0.1 * low, 0.95 * second + 0.05 * low * low


def fused(
    fs_size,
    tp_size,
    input_hbm,
    value_hbm,
    gated_hbm,
    layer_hbm,
    factor_value_hbm,
    factor_output_hbm,
    weight_value_ref,
    weight_output_ref,
    first_value_ref,
    second_value_ref,
    first_output_ref,
    second_output_ref,
    low_ref,
    directions,
    factors,
    scale_ref,
    wide_value_ref,
    wide_output_ref,
    stream,
    cotan,
    projected,
    terms,
    paired,
    outgoing,
    incoming,
    totals,
    load_sem,
    pair_send,
    pair_recv,
    sum_send,
    sum_recv,
    total_send,
    total_recv,
    relay_send,
    relay_recv,
):
    fs, tp = lax.axis_index("fs"), lax.axis_index("tp")
    width = tp_size
    chips = fs_size // CORES
    depth = chips // width
    core, chip = lax.rem(fs, CORES), fs // CORES
    x, z = lax.rem(chip, width), chip // width
    place = (z, x, core, depth, width)
    partner = chip * CORES + 1 - core
    mesh_id = pl.DeviceIdType.MESH
    rows = factor_value_hbm.shape[0]
    tokens = input_hbm.shape[0]
    cols = value_hbm.shape[1]
    ranks = first_value_ref.shape[0]
    everyone = [(a, b) for a in range(fs_size) for b in range(tp_size)][1:]

    own_rows = pl.ds(pl.multiple_of(fs * rows, rows), rows)
    loads = [
        pltpu.make_async_copy(source, target, load_sem.at[slot])
        for slot, (source, target) in enumerate(
            (
                (factor_value_hbm, factors.at[0, own_rows]),
                (factor_output_hbm, factors.at[1, own_rows]),
                (input_hbm, stream.at[0]),
                (layer_hbm, stream.at[1]),
                (value_hbm, cotan.at[0]),
                (gated_hbm, cotan.at[1]),
            )
        )
    ]
    for load in loads:
        load.start()

    barrier = pltpu.get_barrier_semaphore()
    for a, b in everyone:
        pl.semaphore_signal(
            barrier,
            inc=1,
            device_id={"fs": lax.rem(fs + a, fs_size), "tp": lax.rem(tp + b, tp_size)},
            device_id_type=mesh_id,
        )
    loads[0].wait()
    loads[1].wait()
    pl.semaphore_wait(barrier, len(everyone))

    def row_block(ref, size, lead=False):
        def block(origin):
            span = pl.ds(pl.multiple_of(origin * size, size), size)
            return ref.at[:, span] if lead else ref.at[span]

        return block

    half = cols // 2

    def rows_part(part):
        def block(origin):
            span = pl.ds(pl.multiple_of(origin * rows, rows), rows)
            return wide_value_ref.at[span, part * half : (part + 1) * half]

        return block

    def columns_part(part):
        def block(origin):
            span = pl.ds(pl.multiple_of(origin * rows, rows), rows)
            return wide_output_ref.at[part * half : (part + 1) * half, span]

        return block

    gathers = (
        row_block(factors, rows, True),
        row_block(directions, ranks),
        rows_part(0),
        rows_part(1),
        columns_part(0),
        columns_part(1),
    )
    relays = [
        Relay(place, block, relay_send.at[slot], relay_recv.at[slot])
        for slot, block in enumerate(gathers)
    ]

    relays[0].begin()
    wide_value_ref[own_rows, :] = weight_value_ref[...].astype(jnp.bfloat16)
    wide_output_ref[:, own_rows] = weight_output_ref[...].astype(jnp.bfloat16)
    for step in relays[0].middle():
        step()
    relays[2].begin()
    relays[0].finish()
    for load in loads[2:]:
        load.wait()

    tile = 128
    for kind in range(2):

        @pl.loop(0, tokens // tile)
        def _(step, kind=kind):
            span = pl.ds(pl.multiple_of(step * tile, tile), tile)
            projected[kind, span] = jnp.dot(
                stream[kind, span], factors[kind], preferred_element_type=jnp.float32
            ).astype(jnp.bfloat16)

    for step in relays[2].middle():
        step()

    width_tile = 256
    for kind in range(2):

        @pl.loop(0, cols // width_tile)
        def _(step, kind=kind):
            span = pl.ds(pl.multiple_of(step * width_tile, width_tile), width_tile)
            term = lax.dot_general(
                projected[kind],
                cotan[kind, :, span],
                (((0,), (0,)), ((), ())),
                preferred_element_type=jnp.float32,
            )
            target = pl.ds(pl.multiple_of(kind * cols + step * width_tile, width_tile), width_tile)
            terms[:, :, :, target] = term.reshape(chips, CORES, ranks, width_tile)

    pairs = []
    for shift in list(range(1, chips)) + [0]:
        c = lax.rem(chip + shift, chips)
        copy = pltpu.make_async_remote_copy(
            src_ref=terms.at[c, 1 - core],
            dst_ref=paired.at[c],
            send_sem=pair_send.at[shift],
            recv_sem=pair_recv.at[c],
            device_id={"fs": partner},
            device_id_type=mesh_id,
        )
        copy.start()
        pairs.append(copy)
    sums = []
    for shift in range(1, chips):
        c = lax.rem(chip + shift, chips)
        pairs[shift - 1].wait_recv()
        outgoing[c] = (terms[c, core] + paired[c]).astype(jnp.bfloat16)
        copy = pltpu.make_async_remote_copy(
            src_ref=outgoing.at[c],
            dst_ref=incoming.at[chip],
            send_sem=sum_send.at[shift],
            recv_sem=sum_recv.at[chip],
            device_id={"fs": c * CORES + core},
            device_id_type=mesh_id,
        )
        copy.start()
        sums.append(copy)
    relays[3].begin()
    pairs[-1].wait_recv()
    low = terms[chip, core] + paired[chip]
    for shift in range(1, chips):
        c = lax.rem(chip + chips - shift, chips)
        pltpu.make_async_remote_copy(
            src_ref=outgoing.at[c],
            dst_ref=incoming.at[c],
            send_sem=sum_send.at[shift],
            recv_sem=sum_recv.at[c],
            device_id={"fs": c * CORES + core},
            device_id_type=mesh_id,
        ).wait_recv()
        low = low + incoming[c].astype(jnp.float32)

    own_ranks = pl.ds(pl.multiple_of(fs * ranks, ranks), ranks)
    low_ref[...] = low
    moments = ((first_value_ref, second_value_ref), (first_output_ref, second_output_ref))
    for kind, (first_ref, second_ref) in enumerate(moments):
        part = low[:, kind * cols : (kind + 1) * cols]
        next_first, next_second = next_moments(first_ref[...], second_ref[...], part)
        directions[own_ranks, kind * cols : (kind + 1) * cols] = (
            next_first * lax.rsqrt(next_second)
        ).astype(jnp.bfloat16)
    relays[1].begin()
    for first, second in zip(relays[1].middle(), relays[3].middle()):
        first()
        second()
    relays[4].begin()
    relays[5].begin()
    relays[1].finish()

    me = fs * tp_size + tp
    for kind in range(2):
        square = jnp.zeros((8, 128), jnp.float32)
        for start in range(0, cols, width_tile):
            update = jnp.dot(
                factors[kind, own_rows],
                directions[:, kind * cols + start : kind * cols + start + width_tile],
                preferred_element_type=jnp.float32,
            )
            fold = jnp.sum((update * update).reshape(rows // 8, 8, width_tile), axis=0)
            for lane in range(0, width_tile, 128):
                square = square + fold[:, lane : lane + 128]
        totals[me, kind] = square
    shares = []
    for slot, (a, b) in enumerate(everyone):
        copy = pltpu.make_async_remote_copy(
            src_ref=totals.at[me],
            dst_ref=totals.at[me],
            send_sem=total_send.at[slot],
            recv_sem=total_recv.at[me],
            device_id={"fs": lax.rem(fs + a, fs_size), "tp": lax.rem(tp + b, tp_size)},
            device_id_type=mesh_id,
        )
        copy.start()
        shares.append(copy)
    for first, second in zip(relays[4].middle(), relays[5].middle()):
        first()
        second()
    for a, b in everyone:
        other_fs, other_tp = lax.rem(fs + a, fs_size), lax.rem(tp + b, tp_size)
        other = other_fs * tp_size + other_tp
        pltpu.make_async_remote_copy(
            src_ref=totals.at[other],
            dst_ref=totals.at[other],
            send_sem=total_send.at[0],
            recv_sem=total_recv.at[other],
            device_id={"fs": other_fs, "tp": other_tp},
            device_id_type=mesh_id,
        ).wait_recv()
    entries = rows * fs_size * cols * tp_size
    for kind in range(2):
        total = jnp.sum(jnp.sum(totals[:, kind], axis=0), keepdims=True)
        scale = lax.rsqrt(total / entries + 1e-06)
        scale_ref[kind] = jnp.broadcast_to(scale, scale_ref.shape[1:])
    for relay in relays[2:]:
        relay.finish()
    for copy in pairs + sums + shares:
        copy.wait_send()


def apply(
    low_ref,
    directions,
    factors,
    scale_ref,
    wide_value_ref,
    wide_output_ref,
    factor_value_ref,
    factor_output_ref,
    weight_value_ref,
    weight_output_ref,
    first_value_ref,
    second_value_ref,
    first_output_ref,
    second_output_ref,
    step_value_ref,
    step_output_ref,
    next_weight_value_ref,
    next_weight_output_ref,
    next_first_value_ref,
    next_second_value_ref,
    next_first_output_ref,
    next_second_output_ref,
    copy_value_ref,
    copy_output_ref,
    turned,
):
    cols = weight_value_ref.shape[1]
    scale_value, scale_output = scale_ref[0, :1, :1], scale_ref[1, :1, :1]
    last = (((1,), (1,)), ((), ()))

    def update_value(factor):
        return jnp.dot(factor, directions[:, :cols], preferred_element_type=jnp.float32)

    def update_output(factor):
        return lax.dot_general(turned[...], factor, last, preferred_element_type=jnp.float32)

    @pl.when(pl.program_id(0) == 0)
    def _():
        turned[...] = directions[:, cols:].astype(jnp.float32).T.astype(jnp.bfloat16)
        moments = (
            (first_value_ref, second_value_ref, next_first_value_ref, next_second_value_ref),
            (first_output_ref, second_output_ref, next_first_output_ref, next_second_output_ref),
        )
        for kind, (first_ref, second_ref, next_first_ref, next_second_ref) in enumerate(moments):
            next_first_ref[...], next_second_ref[...] = next_moments(
                first_ref[...], second_ref[...], low_ref[:, kind * cols : (kind + 1) * cols]
            )
        step_value = update_value(factor_value_ref[...]) * scale_value
        step_value_ref[...] = step_value
        next_weight_value_ref[...] = weight_value_ref[...] - 0.02 * step_value
        step_output = update_output(factor_output_ref[...]) * scale_output
        step_output_ref[...] = step_output
        next_weight_output_ref[...] = weight_output_ref[...] - 0.02 * step_output

    copy_value_ref[...] = (
        wide_value_ref[...].astype(jnp.float32) - update_value(factors[0]) * (0.02 * scale_value)
    ).astype(jnp.bfloat16)
    copy_output_ref[...] = (
        wide_output_ref[...].astype(jnp.float32) - update_output(factors[1]) * (0.02 * scale_output)
    ).astype(jnp.bfloat16)


def fused_body(fs_size, tp_size, *args):
    tokens, model = args[0].shape
    cols = args[1].shape[1]
    rows, rank = args[4].shape
    ranks = args[8].shape[0]
    chips = fs_size // CORES
    f32, bf16 = jnp.float32, jnp.bfloat16
    vmem, anywhere = pl.BlockSpec(memory_space=pltpu.VMEM), pl.BlockSpec(memory_space=pl.ANY)
    shape = jax.ShapeDtypeStruct
    hops = chips // tp_size - 1 + chips // tp_size + chips
    dma = pltpu.SemaphoreType.DMA
    gathered = pl.pallas_call(
        functools.partial(fused, fs_size, tp_size),
        out_shape=[
            shape((ranks, 2 * cols), f32),
            shape((rank, 2 * cols), bf16),
            shape((2, model, rank), bf16),
            shape((2, 8, 128), f32),
            shape((model, cols), bf16),
            shape((cols, model), bf16),
        ],
        in_specs=[anywhere] * 6 + [vmem] * 6,
        out_specs=[vmem] * 6,
        scratch_shapes=[
            pltpu.VMEM((2, tokens, model), bf16),
            pltpu.VMEM((2, tokens, cols), bf16),
            pltpu.VMEM((2, tokens, rank), bf16),
            pltpu.VMEM((chips, CORES, ranks, 2 * cols), f32),
            pltpu.VMEM((chips, ranks, 2 * cols), f32),
            pltpu.VMEM((chips, ranks, 2 * cols), bf16),
            pltpu.VMEM((chips, ranks, 2 * cols), bf16),
            pltpu.VMEM((fs_size * tp_size, 2, 8, 128), f32),
            dma((6,)),
            dma((chips,)),
            dma((chips,)),
            dma((chips,)),
            dma((chips,)),
            dma((fs_size * tp_size,)),
            dma((fs_size * tp_size,)),
            dma((6, hops)),
            dma((6, fs_size)),
        ],
        compiler_params=pltpu.CompilerParams(
            collective_id=0, has_side_effects=True, vmem_limit_bytes=60 * 1024 * 1024
        ),
    )(*args)

    tile = 2 * rows

    def whole(array):
        return pl.BlockSpec(array.shape, lambda i: (0,) * len(array.shape))

    by_rows = pl.BlockSpec((tile, cols), lambda i: (i, 0))
    by_columns = pl.BlockSpec((cols, tile), lambda i: (0, i))
    own = [shape((rows, cols), f32), shape((cols, rows), f32)] * 2 + [shape((ranks, cols), f32)] * 4
    low, directions, factors, scales = gathered[:4]
    return pl.pallas_call(
        apply,
        grid=(model // tile,),
        out_shape=own + [shape((model, cols), bf16), shape((cols, model), bf16)],
        in_specs=[
            whole(low),
            whole(directions),
            pl.BlockSpec((2, tile, rank), lambda i: (0, i, 0)),
            whole(scales),
            by_rows,
            by_columns,
        ]
        + [whole(array) for array in args[4:]],
        out_specs=[whole(array) for array in own] + [by_rows, by_columns],
        scratch_shapes=[pltpu.VMEM((cols, rank), bf16)],
        compiler_params=pltpu.CompilerParams(vmem_limit_bytes=60 * 1024 * 1024),
    )(*gathered, *args[4:])


def solution(mesh):
    fs_size, tp_size = mesh.shape["fs"], mesh.shape["tp"]
    placed = (
        P("fs", None),
        P("fs", "tp"),
        P("fs", "tp"),
        P("fs", None),
        P("fs", None),
        P("fs", None),
        P("fs", "tp"),
        P("tp", "fs"),
        P("fs", "tp"),
        P("fs", "tp"),
        P("fs", "tp"),
        P("fs", "tp"),
    )
    chips = fs_size // CORES
    tiled = tp_size == 2 and fs_size == 16 and chips % tp_size == 0
    return jax.shard_map(
        functools.partial(fused_body, fs_size, tp_size) if tiled else body,
        mesh=mesh,
        in_specs=placed,
        out_specs=(
            P("fs", "tp"),
            P("tp", "fs"),
            P("fs", "tp"),
            P("tp", "fs"),
            P("fs", "tp"),
            P("fs", "tp"),
            P("fs", "tp"),
            P("fs", "tp"),
            P(None, "tp"),
            P("tp", None),
        ),
        check_vma=False,
    )
```

```python
import functools

import jax
import jax.numpy as jnp
from jax import lax
from jax.experimental import pallas as pl
from jax.experimental.pallas import tpu as pltpu
from jax.sharding import PartitionSpec as P

CORES = 2

D = 2048
WIDTH = 2048


def gram_times(gram_matrix, directions):
    gram_high = gram_matrix.astype(jnp.bfloat16)
    gram_low = (gram_matrix - gram_high.astype(jnp.float32)).astype(jnp.bfloat16)
    return jnp.dot(gram_high, directions, preferred_element_type=jnp.float32) + jnp.dot(
        gram_low, directions, preferred_element_type=jnp.float32
    )


def body(
    normed_input,
    value_cotangent,
    gated_output,
    layer_cotangent,
    factor_value,
    factor_output,
    weight_value,
    weight_output,
    first_value,
    second_value,
    first_output,
    second_output,
):
    col_count = value_cotangent.shape[1]
    inner = (((0,), (0,)), ((), ()))
    pieces = (
        lax.all_gather(factor_value, "fs", axis=0, tiled=True),
        lax.all_gather(factor_output, "fs", axis=0, tiled=True),
    )
    piece_value, piece_output = pieces
    span_input = normed_input
    span_cotan = layer_cotangent
    gram_value = lax.dot_general(pieces[0], pieces[0], inner, preferred_element_type=jnp.float32)
    gram_output = lax.dot_general(pieces[1], pieces[1], inner, preferred_element_type=jnp.float32)
    projected_input = jnp.dot(span_input, piece_value, preferred_element_type=jnp.float32).astype(
        jnp.bfloat16
    )
    projected_cotangent = jnp.dot(
        span_cotan, piece_output, preferred_element_type=jnp.float32
    ).astype(jnp.bfloat16)
    span_input = projected_input
    span_cotan = projected_cotangent
    term_value = lax.dot_general(
        span_input, value_cotangent, inner, preferred_element_type=jnp.float32
    )
    term_output = lax.dot_general(
        span_cotan, gated_output, inner, preferred_element_type=jnp.float32
    )
    low_rank = lax.psum_scatter(
        jnp.concatenate([term_value, term_output], axis=1), "fs", scatter_dimension=0, tiled=True
    )
    low_value = low_rank[:, :col_count]
    low_output = low_rank[:, col_count:]
    next_first_value = 0.9 * first_value + 0.1 * low_value
    next_second_value = 0.95 * second_value + 0.05 * low_value * low_value
    next_first_output = 0.9 * first_output + 0.1 * low_output
    next_second_output = 0.95 * second_output + 0.05 * low_output * low_output
    direction_value = (next_first_value * lax.rsqrt(next_second_value)).astype(jnp.bfloat16)
    direction_output = (next_first_output * lax.rsqrt(next_second_output)).astype(jnp.bfloat16)
    gathered_value, gathered_output = (
        lax.all_gather(direction_value, "fs", axis=0, tiled=True),
        lax.all_gather(direction_output, "fs", axis=0, tiled=True),
    )
    update_value = jnp.dot(factor_value, gathered_value, preferred_element_type=jnp.float32)
    update_output = lax.dot_general(
        gathered_output, factor_output, (((0,), (1,)), ((), ())), preferred_element_type=jnp.float32
    )
    square_value = jnp.sum(
        gathered_value.astype(jnp.float32) * gram_times(gram_value, gathered_value)
    )
    square_output = jnp.sum(
        gathered_output.astype(jnp.float32) * gram_times(gram_output, gathered_output)
    )
    total_value, total_output = lax.psum((square_value, square_output), "tp")
    entries = D * WIDTH
    step_value = update_value * lax.rsqrt(total_value / entries + 1e-06)
    step_output = update_output * lax.rsqrt(total_output / entries + 1e-06)
    next_weight_value = weight_value - 0.02 * step_value
    next_weight_output = weight_output - 0.02 * step_output
    half_value = next_weight_value.astype(jnp.bfloat16)
    half_output = next_weight_output.astype(jnp.bfloat16)
    copy_value, copy_output = (
        lax.all_gather(half_value, "fs", axis=0, tiled=True),
        lax.all_gather(half_output, "fs", axis=1, tiled=True),
    )
    return (
        step_value,
        step_output,
        next_weight_value,
        next_weight_output,
        next_first_value,
        next_second_value,
        next_first_output,
        next_second_output,
        copy_value,
        copy_output,
    )


class Relay:
    def __init__(self, place, block, send_sem, recv_sem):
        self.z, self.x, self.core, self.depth, self.width = place
        self.block, self.send_sem, self.recv_sem = block, send_sem, recv_sem
        self.pending = []

    def index(self, shift, x, core):
        z = lax.rem(self.z + shift, self.depth)
        return (z * self.width + x) * CORES + core

    def copy(self, origin, target, slot):
        return pltpu.make_async_remote_copy(
            src_ref=self.block(origin),
            dst_ref=self.block(origin),
            send_sem=self.send_sem.at[slot],
            recv_sem=self.recv_sem.at[origin],
            device_id={"fs": target},
            device_id_type=pl.DeviceIdType.MESH,
        )

    def send(self, origin, target):
        copy = self.copy(origin, target, len(self.pending))
        copy.start()
        self.pending.append(copy)

    def arrived(self, origin):
        self.copy(origin, self.index(0, self.x, 1 - self.core), 0).wait_recv()

    def over_x(self, origin):
        self.send(origin, self.index(0, 1 - self.x, self.core))

    def over_core(self, origin):
        self.send(origin, self.index(0, self.x, 1 - self.core))

    def order(self):
        shifts = []
        for hop in range(1, self.depth // 2 + 1):
            for shift in (hop, self.depth - hop):
                if shift not in shifts:
                    shifts.append(shift)
        return shifts

    def begin(self):
        own = self.index(0, self.x, self.core)
        for shift in self.order():
            self.send(own, self.index(shift, self.x, self.core))
        self.over_x(own)
        self.over_core(own)

    def along_z(self, shift):
        origin = self.index(shift, self.x, self.core)
        self.arrived(origin)
        self.over_x(origin)
        self.over_core(origin)

    def across(self, shift):
        origin = self.index(shift, 1 - self.x, self.core)
        self.arrived(origin)
        self.over_core(origin)

    def middle(self):
        lagged = [0]
        for shift in self.order():
            yield functools.partial(self.along_z, shift)
            lagged.append(shift)
            if len(lagged) > 1:
                yield functools.partial(self.across, lagged.pop(0))
        for shift in lagged:
            yield functools.partial(self.across, shift)

    def finish(self):
        for shift in [0] + self.order():
            for x in (self.x, 1 - self.x):
                self.arrived(self.index(shift, x, 1 - self.core))
        for copy in self.pending:
            copy.wait_send()


def next_moments(first, second, low):
    return 0.9 * first + 0.1 * low, 0.95 * second + 0.05 * low * low


def fused(
    fs_size,
    tp_size,
    input_hbm,
    value_hbm,
    gated_hbm,
    layer_hbm,
    factor_value_hbm,
    factor_output_hbm,
    weight_value_ref,
    weight_output_ref,
    first_value_ref,
    second_value_ref,
    first_output_ref,
    second_output_ref,
    low_ref,
    directions,
    factors,
    scale_ref,
    wide_value_ref,
    wide_output_ref,
    stream,
    cotan,
    projected,
    terms,
    paired,
    outgoing,
    incoming,
    totals,
    load_sem,
    pair_send,
    pair_recv,
    sum_send,
    sum_recv,
    total_send,
    total_recv,
    relay_send,
    relay_recv,
):
    fs, tp = lax.axis_index("fs"), lax.axis_index("tp")
    width = tp_size
    chips = fs_size // CORES
    depth = chips // width
    core, chip = lax.rem(fs, CORES), fs // CORES
    x, z = lax.rem(chip, width), chip // width
    place = (z, x, core, depth, width)
    partner = chip * CORES + 1 - core
    mesh_id = pl.DeviceIdType.MESH
    rows = factor_value_hbm.shape[0]
    tokens = input_hbm.shape[0]
    cols = value_hbm.shape[1]
    ranks = first_value_ref.shape[0]
    everyone = [(a, b) for a in range(fs_size) for b in range(tp_size)][1:]

    own_rows = pl.ds(pl.multiple_of(fs * rows, rows), rows)
    loads = [
        pltpu.make_async_copy(source, target, load_sem.at[slot])
        for slot, (source, target) in enumerate(
            (
                (factor_value_hbm, factors.at[0, own_rows]),
                (factor_output_hbm, factors.at[1, own_rows]),
                (input_hbm, stream.at[0]),
                (layer_hbm, stream.at[1]),
                (value_hbm, cotan.at[0]),
                (gated_hbm, cotan.at[1]),
            )
        )
    ]
    for load in loads:
        load.start()

    barrier = pltpu.get_barrier_semaphore()
    for a, b in everyone:
        pl.semaphore_signal(
            barrier,
            inc=1,
            device_id={"fs": lax.rem(fs + a, fs_size), "tp": lax.rem(tp + b, tp_size)},
            device_id_type=mesh_id,
        )
    loads[0].wait()
    loads[1].wait()
    pl.semaphore_wait(barrier, len(everyone))

    def row_block(ref, size, lead=False):
        def block(origin):
            span = pl.ds(pl.multiple_of(origin * size, size), size)
            return ref.at[:, span] if lead else ref.at[span]

        return block

    half = cols // 2

    def rows_part(part):
        def block(origin):
            span = pl.ds(pl.multiple_of(origin * rows, rows), rows)
            return wide_value_ref.at[span, part * half : (part + 1) * half]

        return block

    def columns_part(part):
        def block(origin):
            span = pl.ds(pl.multiple_of(origin * rows, rows), rows)
            return wide_output_ref.at[part * half : (part + 1) * half, span]

        return block

    gathers = (
        row_block(factors, rows, True),
        row_block(directions, ranks),
        rows_part(0),
        rows_part(1),
        columns_part(0),
        columns_part(1),
    )
    relays = [
        Relay(place, block, relay_send.at[slot], relay_recv.at[slot])
        for slot, block in enumerate(gathers)
    ]

    relays[0].begin()
    wide_value_ref[own_rows, :] = weight_value_ref[...].astype(jnp.bfloat16)
    wide_output_ref[:, own_rows] = weight_output_ref[...].astype(jnp.bfloat16)
    for step in relays[0].middle():
        step()
    relays[2].begin()
    relays[0].finish()
    for load in loads[2:]:
        load.wait()

    tile = 128
    for kind in range(2):

        @pl.loop(0, tokens // tile)
        def _(step, kind=kind):
            span = pl.ds(pl.multiple_of(step * tile, tile), tile)
            projected[kind, span] = jnp.dot(
                stream[kind, span], factors[kind], preferred_element_type=jnp.float32
            ).astype(jnp.bfloat16)

    width_tile = 256
    for kind in range(2):

        @pl.loop(0, cols // width_tile)
        def _(step, kind=kind):
            span = pl.ds(pl.multiple_of(step * width_tile, width_tile), width_tile)
            term = lax.dot_general(
                projected[kind],
                cotan[kind, :, span],
                (((0,), (0,)), ((), ())),
                preferred_element_type=jnp.float32,
            )
            target = pl.ds(pl.multiple_of(kind * cols + step * width_tile, width_tile), width_tile)
            terms[:, :, :, target] = term.reshape(chips, CORES, ranks, width_tile)

    pairs = []
    for shift in list(range(1, chips)) + [0]:
        c = lax.rem(chip + shift, chips)
        copy = pltpu.make_async_remote_copy(
            src_ref=terms.at[c, 1 - core],
            dst_ref=paired.at[c],
            send_sem=pair_send.at[shift],
            recv_sem=pair_recv.at[c],
            device_id={"fs": partner},
            device_id_type=mesh_id,
        )
        copy.start()
        pairs.append(copy)
    sums = []
    for shift in range(1, chips):
        c = lax.rem(chip + shift, chips)
        pairs[shift - 1].wait_recv()
        outgoing[c] = (terms[c, core] + paired[c]).astype(jnp.bfloat16)
        copy = pltpu.make_async_remote_copy(
            src_ref=outgoing.at[c],
            dst_ref=incoming.at[chip],
            send_sem=sum_send.at[shift],
            recv_sem=sum_recv.at[chip],
            device_id={"fs": c * CORES + core},
            device_id_type=mesh_id,
        )
        copy.start()
        sums.append(copy)
    for step in relays[2].middle():
        step()
    relays[3].begin()
    pairs[-1].wait_recv()
    low = terms[chip, core] + paired[chip]
    for shift in range(1, chips):
        c = lax.rem(chip + chips - shift, chips)
        pltpu.make_async_remote_copy(
            src_ref=outgoing.at[c],
            dst_ref=incoming.at[c],
            send_sem=sum_send.at[shift],
            recv_sem=sum_recv.at[c],
            device_id={"fs": c * CORES + core},
            device_id_type=mesh_id,
        ).wait_recv()
        low = low + incoming[c].astype(jnp.float32)

    own_ranks = pl.ds(pl.multiple_of(fs * ranks, ranks), ranks)
    low_ref[...] = low
    moments = ((first_value_ref, second_value_ref), (first_output_ref, second_output_ref))
    for kind, (first_ref, second_ref) in enumerate(moments):
        part = low[:, kind * cols : (kind + 1) * cols]
        next_first, next_second = next_moments(first_ref[...], second_ref[...], part)
        directions[own_ranks, kind * cols : (kind + 1) * cols] = (
            next_first * lax.rsqrt(next_second)
        ).astype(jnp.bfloat16)
    relays[1].begin()
    for first, second in zip(relays[1].middle(), relays[3].middle()):
        first()
        second()
    relays[4].begin()
    relays[5].begin()
    relays[1].finish()

    me = fs * tp_size + tp
    for kind in range(2):
        square = jnp.zeros((8, 128), jnp.float32)
        for start in range(0, cols, width_tile):
            update = jnp.dot(
                factors[kind, own_rows],
                directions[:, kind * cols + start : kind * cols + start + width_tile],
                preferred_element_type=jnp.float32,
            )
            fold = jnp.sum((update * update).reshape(rows // 8, 8, width_tile), axis=0)
            for lane in range(0, width_tile, 128):
                square = square + fold[:, lane : lane + 128]
        totals[me, kind] = square
    shares = []
    for slot, (a, b) in enumerate(everyone):
        copy = pltpu.make_async_remote_copy(
            src_ref=totals.at[me],
            dst_ref=totals.at[me],
            send_sem=total_send.at[slot],
            recv_sem=total_recv.at[me],
            device_id={"fs": lax.rem(fs + a, fs_size), "tp": lax.rem(tp + b, tp_size)},
            device_id_type=mesh_id,
        )
        copy.start()
        shares.append(copy)
    for first, second in zip(relays[4].middle(), relays[5].middle()):
        first()
        second()
    for a, b in everyone:
        other_fs, other_tp = lax.rem(fs + a, fs_size), lax.rem(tp + b, tp_size)
        other = other_fs * tp_size + other_tp
        pltpu.make_async_remote_copy(
            src_ref=totals.at[other],
            dst_ref=totals.at[other],
            send_sem=total_send.at[0],
            recv_sem=total_recv.at[other],
            device_id={"fs": other_fs, "tp": other_tp},
            device_id_type=mesh_id,
        ).wait_recv()
    entries = rows * fs_size * cols * tp_size
    for kind in range(2):
        total = jnp.sum(jnp.sum(totals[:, kind], axis=0), keepdims=True)
        scale = lax.rsqrt(total / entries + 1e-06)
        scale_ref[kind] = jnp.broadcast_to(scale, scale_ref.shape[1:])
    for relay in relays[2:]:
        relay.finish()
    for copy in pairs + sums + shares:
        copy.wait_send()


def apply(
    low_ref,
    directions,
    factors,
    scale_ref,
    wide_value_ref,
    wide_output_ref,
    factor_value_ref,
    factor_output_ref,
    weight_value_ref,
    weight_output_ref,
    first_value_ref,
    second_value_ref,
    first_output_ref,
    second_output_ref,
    step_value_ref,
    step_output_ref,
    next_weight_value_ref,
    next_weight_output_ref,
    next_first_value_ref,
    next_second_value_ref,
    next_first_output_ref,
    next_second_output_ref,
    copy_value_ref,
    copy_output_ref,
    turned,
):
    cols = weight_value_ref.shape[1]
    scale_value, scale_output = scale_ref[0, :1, :1], scale_ref[1, :1, :1]
    last = (((1,), (1,)), ((), ()))

    def update_value(factor):
        return jnp.dot(factor, directions[:, :cols], preferred_element_type=jnp.float32)

    def update_output(factor):
        return lax.dot_general(turned[...], factor, last, preferred_element_type=jnp.float32)

    @pl.when(pl.program_id(0) == 0)
    def _():
        turned[...] = directions[:, cols:].astype(jnp.float32).T.astype(jnp.bfloat16)
        moments = (
            (first_value_ref, second_value_ref, next_first_value_ref, next_second_value_ref),
            (first_output_ref, second_output_ref, next_first_output_ref, next_second_output_ref),
        )
        for kind, (first_ref, second_ref, next_first_ref, next_second_ref) in enumerate(moments):
            next_first_ref[...], next_second_ref[...] = next_moments(
                first_ref[...], second_ref[...], low_ref[:, kind * cols : (kind + 1) * cols]
            )
        step_value = update_value(factor_value_ref[...]) * scale_value
        step_value_ref[...] = step_value
        next_weight_value_ref[...] = weight_value_ref[...] - 0.02 * step_value
        step_output = update_output(factor_output_ref[...]) * scale_output
        step_output_ref[...] = step_output
        next_weight_output_ref[...] = weight_output_ref[...] - 0.02 * step_output

    copy_value_ref[...] = (
        wide_value_ref[...].astype(jnp.float32) - update_value(factors[0]) * (0.02 * scale_value)
    ).astype(jnp.bfloat16)
    copy_output_ref[...] = (
        wide_output_ref[...].astype(jnp.float32) - update_output(factors[1]) * (0.02 * scale_output)
    ).astype(jnp.bfloat16)


def fused_body(fs_size, tp_size, *args):
    tokens, model = args[0].shape
    cols = args[1].shape[1]
    rows, rank = args[4].shape
    ranks = args[8].shape[0]
    chips = fs_size // CORES
    f32, bf16 = jnp.float32, jnp.bfloat16
    vmem, anywhere = pl.BlockSpec(memory_space=pltpu.VMEM), pl.BlockSpec(memory_space=pl.ANY)
    shape = jax.ShapeDtypeStruct
    hops = chips // tp_size - 1 + chips // tp_size + chips
    dma = pltpu.SemaphoreType.DMA
    gathered = pl.pallas_call(
        functools.partial(fused, fs_size, tp_size),
        out_shape=[
            shape((ranks, 2 * cols), f32),
            shape((rank, 2 * cols), bf16),
            shape((2, model, rank), bf16),
            shape((2, 8, 128), f32),
            shape((model, cols), bf16),
            shape((cols, model), bf16),
        ],
        in_specs=[anywhere] * 6 + [vmem] * 6,
        out_specs=[vmem] * 6,
        scratch_shapes=[
            pltpu.VMEM((2, tokens, model), bf16),
            pltpu.VMEM((2, tokens, cols), bf16),
            pltpu.VMEM((2, tokens, rank), bf16),
            pltpu.VMEM((chips, CORES, ranks, 2 * cols), f32),
            pltpu.VMEM((chips, ranks, 2 * cols), f32),
            pltpu.VMEM((chips, ranks, 2 * cols), bf16),
            pltpu.VMEM((chips, ranks, 2 * cols), bf16),
            pltpu.VMEM((fs_size * tp_size, 2, 8, 128), f32),
            dma((6,)),
            dma((chips,)),
            dma((chips,)),
            dma((chips,)),
            dma((chips,)),
            dma((fs_size * tp_size,)),
            dma((fs_size * tp_size,)),
            dma((6, hops)),
            dma((6, fs_size)),
        ],
        compiler_params=pltpu.CompilerParams(
            collective_id=0, has_side_effects=True, vmem_limit_bytes=60 * 1024 * 1024
        ),
    )(*args)

    tile = 2 * rows

    def whole(array):
        return pl.BlockSpec(array.shape, lambda i: (0,) * len(array.shape))

    by_rows = pl.BlockSpec((tile, cols), lambda i: (i, 0))
    by_columns = pl.BlockSpec((cols, tile), lambda i: (0, i))
    own = [shape((rows, cols), f32), shape((cols, rows), f32)] * 2 + [shape((ranks, cols), f32)] * 4
    low, directions, factors, scales = gathered[:4]
    return pl.pallas_call(
        apply,
        grid=(model // tile,),
        out_shape=own + [shape((model, cols), bf16), shape((cols, model), bf16)],
        in_specs=[
            whole(low),
            whole(directions),
            pl.BlockSpec((2, tile, rank), lambda i: (0, i, 0)),
            whole(scales),
            by_rows,
            by_columns,
        ]
        + [whole(array) for array in args[4:]],
        out_specs=[whole(array) for array in own] + [by_rows, by_columns],
        scratch_shapes=[pltpu.VMEM((cols, rank), bf16)],
        compiler_params=pltpu.CompilerParams(vmem_limit_bytes=60 * 1024 * 1024),
    )(*gathered, *args[4:])


def solution(mesh):
    fs_size, tp_size = mesh.shape["fs"], mesh.shape["tp"]
    placed = (
        P("fs", None),
        P("fs", "tp"),
        P("fs", "tp"),
        P("fs", None),
        P("fs", None),
        P("fs", None),
        P("fs", "tp"),
        P("tp", "fs"),
        P("fs", "tp"),
        P("fs", "tp"),
        P("fs", "tp"),
        P("fs", "tp"),
    )
    chips = fs_size // CORES
    tiled = tp_size == 2 and fs_size == 16 and chips % tp_size == 0
    return jax.shard_map(
        functools.partial(fused_body, fs_size, tp_size) if tiled else body,
        mesh=mesh,
        in_specs=placed,
        out_specs=(
            P("fs", "tp"),
            P("tp", "fs"),
            P("fs", "tp"),
            P("tp", "fs"),
            P("fs", "tp"),
            P("fs", "tp"),
            P("fs", "tp"),
            P("fs", "tp"),
            P(None, "tp"),
            P("tp", None),
        ),
        check_vma=False,
    )
```
